32 devices in a mesh: grp: 2 (over x), ep: 4 (over y, core), tp: 4 (over z).
Axes of the slice: x: 2, y: 2, z: 4, core: 2. Of those that a mesh axis runs over, the one named last changes fastest.
Arguments:
- tokens: bfloat16 [2048, 4096], P(('grp', 'ep')), parts along dimension 0, may hold values from -6 to 6
- expert_ids: int32 [2048, 2], P(('grp', 'ep')), parts along dimension 0, may hold values from 0 to 15, as said below
- gates: float32 [2048, 2], P(('grp', 'ep')), parts along dimension 0, may hold values from 0.1 to 1
- w_gate: bfloat16 [16, 4096, 2048], P('ep', None, 'tp'), may hold values from -0.09375 to 0.09375
- w_up: bfloat16 [16, 4096, 2048], P('ep', None, 'tp'), may hold values from -0.09375 to 0.09375
- w_down: bfloat16 [16, 2048, 4096], P('ep', 'tp'), may hold values from -0.79549513 to 0.79549513, as said below
- norm_gain: float32 [4096], P('tp'), may hold values from 0.1 to 1.9
- norm_bias: float32 [4096], P('tp'), may hold values from -1.5 to 1.5
Outputs:
- normed: bfloat16 [2048, 4096], P(('grp', 'ep'), 'tp'), parts along dimension 0
The draws below stay inside these ranges and needn't reach their ends.
There are 2 independent parts, one for each index of `grp`. The reference program is written for one: setup_inputs(seed, part) draws one part's arguments, and reference() takes and returns one part's arrays. A program takes and returns all parts, laid end to end along the dimension named above; an argument that names none is the same for every part. Nothing has to cross between parts.
Inputs may be any that keep to these rules, and one draw needn't show every extreme that they name: `expert_ids`: each row names 2 different experts, both in the same group of 4 consecutive expert numbers. Within one aligned block of 256 rows no expert is named more than 64 times, and in every draw some expert is named exactly 64 times in every block. `w_down`: down projection weights.
All inputs are finite; a program needn't handle non-finite values.
Results may differ from the reference program's by a relative error of at most 0.014.
Values may be sent and summed in bfloat16 or wider, within the bound.
A program may use at most 128 MiB of HBM per device.

```python
import math
import jax
import jax.numpy as jnp
from jax import lax

D = 4096
FF = 2048
GROUPS = 4
EXPERTS_PER_GROUP = 4
TOPK = 2
TOK_DEV = 256
EXPERTS = 16
CAP = 64
SLOTS = 256
FF_DEV = 512
TOKENS = 1024
N_EP = 4
N_TP = 4


def route_block(block_key, busy_group):
    key_weights, key_labels, key_shuffle = jax.random.split(block_key, 3)
    weights = jax.random.randint(key_weights, (GROUPS,), 4, 9)
    is_busy = jnp.arange(GROUPS) == busy_group
    weights = jnp.where(is_busy, 0, weights)
    busy_count = TOK_DEV // 2
    remainder = TOK_DEV - busy_count
    counts = remainder * weights // jnp.sum(weights)
    leftover = remainder - jnp.sum(counts)
    first_other = jnp.argmin(is_busy.astype(jnp.int32))
    counts = counts + leftover * (jnp.arange(GROUPS) == first_other).astype(jnp.int32)
    counts = jnp.where(is_busy, busy_count, counts)
    group_ends = jnp.cumsum(counts)
    group_starts = group_ends - counts
    position = jnp.arange(TOK_DEV)
    group_of = jnp.sum((position[:, None] >= group_ends[None, :]).astype(jnp.int32), axis=1)
    within = position - group_starts[group_of]
    first_table = jnp.array([0, 2, 0, 1, 0, 1], jnp.int32)
    second_table = jnp.array([1, 3, 2, 3, 3, 2], jnp.int32)
    relabel = jax.vmap(lambda label_key: jax.random.permutation(label_key, EXPERTS_PER_GROUP))(jax.random.split(key_labels, GROUPS))
    group_base = group_of * EXPERTS_PER_GROUP
    first_expert = group_base + relabel[group_of, first_table[within % 6]]
    second_expert = group_base + relabel[group_of, second_table[within % 6]]
    chosen = jnp.stack([first_expert, second_expert], axis=1).astype(jnp.int32)
    shuffle = jax.random.permutation(key_shuffle, TOK_DEV)
    return chosen[shuffle]


def draw_expert_ids(key, part):
    busy_group = jax.random.randint(jax.random.fold_in(key, 7), (), 0, GROUPS)
    block_keys = jax.random.split(jax.random.fold_in(key, 11), TOKENS // TOK_DEV)
    chosen = jax.vmap(route_block, in_axes=(0, None))(block_keys, busy_group)
    return chosen.reshape(TOKENS, TOPK).astype(jnp.int32)


def draw_w_down(key, part):
    noise = jnp.clip(jax.random.normal(jax.random.fold_in(key, 3), (EXPERTS, FF, D), jnp.float32), -6.0, 6.0)
    columns = 0.6 * jnp.exp(math.log(3.0) * jnp.arange(D, dtype=jnp.float32) / (D - 1))
    return (noise * FF ** (-0.5) * columns).astype(jnp.bfloat16)


def shard_levels(key, extent, shards, low, top_value):
    gain = 1.0
    for dim, shards_of in shards:
        draws = jax.random.uniform(jax.random.fold_in(jax.random.fold_in(key, 6), dim), (shards_of,), jnp.float32, low / len(shards), top_value / len(shards))
        gain = gain * jnp.repeat(jnp.exp(draws), extent[dim] // shards_of).reshape((-1,) + (1,) * (len(extent) - 1 - dim))
    return gain


def normal_values(key, shape, width, limit, cuts=(), kind=jnp.bfloat16):
    drawn = width * jax.random.normal(key, shape, jnp.float32)
    if cuts:
        drawn = drawn * shard_levels(key, shape, cuts, -0.22, 0.18)
    return jnp.clip(drawn, -limit, limit).astype(kind)


def setup_inputs(seed: int = 0, part: int = 0) -> dict:
    seeds = jax.random.split(jax.random.key(seed), 9)
    part_splits = jax.random.split(jax.random.fold_in(seeds[8], part), 9)
    tokens = normal_values(part_splits[0], (TOKENS, D), 1.0, 6.0, ((0, 4),))
    expert_ids = draw_expert_ids(jax.random.fold_in(jax.random.fold_in(seeds[8], part), 71), part)
    gates = jnp.clip(0.1 + 0.9 * jax.random.uniform(part_splits[2], (TOKENS, TOPK), jnp.float32) ** shard_levels(part_splits[2], (TOKENS, TOPK), ((0, 4),), -0.2, 0.2), 0.1, 1.0)
    w_gate = normal_values(seeds[3], (EXPERTS, D, FF), D ** -0.5, 0.09375, ((0, 4), (2, 4)))
    w_up = normal_values(seeds[4], (EXPERTS, D, FF), D ** -0.5, 0.09375, ((0, 4), (2, 4)))
    w_down = draw_w_down(jax.random.fold_in(seeds[8], 71), part)
    norm_gain = jnp.clip(1.0 + 0.18 * jax.random.normal(seeds[6], (D,), jnp.float32), 0.1, 1.9)
    norm_bias = normal_values(seeds[7], (D,), 0.3, 1.5, ((0, 4),), jnp.float32)
    return dict(tokens=tokens, expert_ids=expert_ids, gates=gates, w_gate=w_gate, w_up=w_up, w_down=w_down, norm_gain=norm_gain, norm_bias=norm_bias)


norm_eps = 1e-05

def run_expert(operands):
    routed, gate_w, up_w, down_w = operands
    gate_part = jnp.dot(routed, gate_w, preferred_element_type=jnp.float32)
    up_part = jnp.dot(routed, up_w, preferred_element_type=jnp.float32)
    hidden = (jax.nn.silu(gate_part) * up_part).astype(jnp.bfloat16)
    blocks = hidden.reshape(SLOTS, N_TP, FF_DEV).astype(jnp.float32)
    down_blocks = down_w.reshape(N_TP, FF_DEV, D).astype(jnp.float32)
    partial_value = jnp.einsum('rjf,jfd->jrd', blocks, down_blocks).astype(jnp.bfloat16)
    partial_value = lax.optimization_barrier(partial_value)
    return lax.optimization_barrier(jnp.sum(partial_value.astype(jnp.float32), axis=0)).astype(jnp.bfloat16)

def reference(tokens, expert_ids, gates, w_gate, w_up, w_down, norm_gain, norm_bias):
    flat_ids = expert_ids.reshape(N_EP, TOK_DEV * TOPK)
    onehot = (flat_ids[:, :, None] == jnp.arange(EXPERTS, dtype=jnp.int32)[None, None, :]).astype(jnp.int32)
    position = lax.optimization_barrier(jnp.sum((jnp.cumsum(onehot, axis=1) - 1) * onehot, axis=2))
    source_block = jnp.arange(N_EP, dtype=jnp.int32)[:, None]
    target = (flat_ids * SLOTS + source_block * CAP + position).reshape(-1).astype(jnp.int32)
    token_of = jnp.arange(TOKENS * TOPK, dtype=jnp.int32) // TOPK
    source = jnp.zeros((EXPERTS * SLOTS,), jnp.int32).at[target].set(token_of)
    filled = jnp.zeros((EXPERTS * SLOTS,), jnp.bool_).at[target].set(True)
    routed = jnp.where(filled[:, None], tokens[source], jnp.zeros((), jnp.bfloat16)).reshape(EXPERTS, SLOTS, D)
    expert_out = lax.map(run_expert, (routed, w_gate, w_up, w_down))
    picked = expert_out.reshape(EXPERTS * SLOTS, D)[target].reshape(TOKENS, TOPK, D)
    combined = lax.optimization_barrier(jnp.sum(picked.astype(jnp.float32) * gates[:, :, None], axis=1))
    row_mean = lax.optimization_barrier(jnp.mean(combined, axis=1, keepdims=True))
    centred = combined - row_mean
    row_var = lax.optimization_barrier(jnp.mean(centred * centred, axis=1, keepdims=True))
    normed = centred * lax.rsqrt(row_var + norm_eps) * norm_gain + norm_bias
    return normed.astype(jnp.bfloat16)
```

```python
import functools
import jax
import jax.numpy as jnp
from jax import lax
from jax.experimental import pallas as pl
from jax.experimental.pallas import tpu as pltpu
from jax.sharding import PartitionSpec as P

D = 4096
TOPK = 2
EXPERTS = 16
CAP = 64


norm_eps = 1e-05


def route_slots(expert_ids):
    flat_ids = expert_ids.reshape(-1)
    onehot = (flat_ids[:, None] == jnp.arange(EXPERTS, dtype=jnp.int32)[None, :]).astype(jnp.int32)
    position = jnp.sum((jnp.cumsum(onehot, axis=0) - 1) * onehot, axis=1)
    target = flat_ids * CAP + position
    token_of = jnp.arange(flat_ids.shape[0], dtype=jnp.int32) // TOPK
    source = jnp.zeros((EXPERTS * CAP,), jnp.int32).at[target].set(token_of)
    filled = jnp.zeros((EXPERTS * CAP,), jnp.bool_).at[target].set(True)
    return (target, source, filled)


def on_device(tokens, expert_ids, gates, w_gate, w_up, w_down, norm_gain, norm_bias):
    tok_rows, width = tokens.shape
    piece_width = norm_gain.shape[0]
    target, source, filled = route_slots(expert_ids)
    outgoing = jnp.where(filled[:, None], tokens[source], jnp.zeros((), jnp.bfloat16)).reshape(
        EXPERTS, CAP, width
    )
    arrived = lax.all_to_all(outgoing, "ep", split_axis=0, concat_axis=1, tiled=True)
    gate_part = jnp.einsum("erd,edf->erf", arrived, w_gate, preferred_element_type=jnp.float32)
    up_part = jnp.einsum("erd,edf->erf", arrived, w_up, preferred_element_type=jnp.float32)
    hidden = (jax.nn.silu(gate_part) * up_part).astype(jnp.bfloat16)
    partial_value = jnp.einsum("erf,efd->erd", hidden, w_down, preferred_element_type=jnp.float32)
    summed = lax.psum_scatter(
        partial_value.astype(jnp.bfloat16), "tp", scatter_dimension=2, tiled=True
    )
    returned = lax.all_to_all(summed, "ep", split_axis=1, concat_axis=0, tiled=True)
    picked = returned.reshape(EXPERTS * CAP, piece_width)[target].reshape(
        tok_rows, TOPK, piece_width
    )
    combined = jnp.sum(picked.astype(jnp.float32) * gates[:, :, None], axis=1)
    stats = lax.psum((jnp.sum(combined, axis=1), jnp.sum(combined * combined, axis=1)), "tp")
    row_mean = stats[0] / D
    row_var = stats[1] / D - row_mean * row_mean
    normed = (combined - row_mean[:, None]) * lax.rsqrt(
        row_var[:, None] + norm_eps
    ) * norm_gain + norm_bias
    return normed.astype(jnp.bfloat16)


GROUP_EXPERTS = 4
CHUNKS = 8
HALF = CHUNKS // 2
Z_OFFSETS = (2, 1, 3, 0)
F32 = jnp.float32
BF16 = jnp.bfloat16
MESH = pl.DeviceIdType.MESH


def moe_kernel(
    ids_ref, gates_ref, gain_ref, bias_ref, tokens_ref, wg_ref, wu_ref, wd_ref,
    out_ref,
    tok, wbuf, wd, acc, hid, xr, dnb, place, collect, rowg, meta, meta_in,
    part, core_in, y_in, z_in, st_out, st_in,
    tok_sem, y_send, y_recv, z_send, z_recv, own_send, own_recv, fwd_send, fwd_recv,
    meta_send, meta_recv, w_sem, wd_sem, pc_send, pc_recv, py_send, py_recv,
    pz_send, pz_recv, st_send, st_recv,
):
    ep = lax.axis_index("ep")
    z = lax.axis_index("tp")
    y, c = ep // 2, ep % 2
    partner = y * 2 + (1 - c)
    across = (1 - y) * 2 + c
    diag = (1 - y) * 2 + (1 - c)
    par = z % 2
    zpeer = z + 1 - 2 * par
    rows, width = tokens_ref.shape
    experts = wg_ref.shape[0]
    cols = width // CHUNKS
    piece = gain_ref.shape[1]

    def remote(src, dst, send, recv, e, t):
        return pltpu.make_async_remote_copy(
            src_ref=src, dst_ref=dst, send_sem=send, recv_sem=recv,
            device_id={"ep": e, "tp": t}, device_id_type=MESH,
        )

    def span(ch, size):
        return pl.ds(pl.multiple_of(ch * size, size), size)

    def load_tok(ch):
        return pltpu.make_async_copy(
            tokens_ref.at[:, span(ch, cols)], tok.at[ch, ep], tok_sem.at[ch])

    def load_w(ch, slot):
        return (
            pltpu.make_async_copy(
                wg_ref.at[:, span(ch, cols), :], wbuf.at[slot, 0], w_sem.at[slot, 0]),
            pltpu.make_async_copy(
                wu_ref.at[:, span(ch, cols), :], wbuf.at[slot, 1], w_sem.at[slot, 1]),
        )

    def load_wd(i):
        q = (z + Z_OFFSETS[i]) % 4
        return pltpu.make_async_copy(
            wd_ref.at[:, :, span(q, piece)], wd.at[i], wd_sem.at[i])

    def direct(j):
        return par * HALF + j

    def swapped(j):
        return (1 - par) * HALF + j

    def y_copy(j):
        blk = tok.at[direct(j), ep]
        return remote(blk, blk, y_send.at[j], y_recv.at[j], across, z)

    def y_arrive(j):
        blk = tok.at[direct(j), across]
        return remote(blk, blk, y_send.at[j], y_recv.at[j], across, z)

    def z_copy(j):
        blk = tok.at[direct(j), across]
        return remote(blk, blk, z_send.at[j], z_recv.at[j], ep, zpeer)

    def z_arrive(j):
        blk = tok.at[swapped(j), across]
        return remote(blk, blk, z_send.at[j], z_recv.at[j], ep, zpeer)

    def own_copy(ch):
        blk = tok.at[ch, ep]
        return remote(blk, blk, own_send.at[ch], own_recv.at[ch], partner, z)

    def own_arrive(ch):
        blk = tok.at[ch, partner]
        return remote(blk, blk, own_send.at[ch], own_recv.at[ch], partner, z)

    def fwd_copy(ch):
        blk = tok.at[ch, across]
        return remote(blk, blk, fwd_send.at[ch], fwd_recv.at[ch], partner, z)

    def fwd_arrive(ch):
        blk = tok.at[ch, diag]
        return remote(blk, blk, fwd_send.at[ch], fwd_recv.at[ch], partner, z)

    def meta_copy(e, k):
        return remote(meta.at[e], meta_in.at[ep], meta_send.at[k], meta_recv.at[k], e, z)

    def meta_arrive(e, k):
        return remote(meta.at[e], meta_in.at[e], meta_send.at[k], meta_recv.at[k], e, z)

    peers = (partner, across, diag)

    for j in range(HALF):
        load_tok(direct(j)).start()
    for j in range(HALF):
        load_tok(swapped(j)).start()

    barrier = pltpu.get_barrier_semaphore()
    for e in peers:
        pl.semaphore_signal(barrier, inc=1, device_id={"ep": e, "tp": z}, device_id_type=MESH)
    for d in (1, 2, 3):
        pl.semaphore_signal(
            barrier, inc=1, device_id={"ep": ep, "tp": (z + d) % 4}, device_id_type=MESH)
    pl.semaphore_wait(barrier, 6)

    for j in range(HALF):
        load_tok(direct(j)).wait()
        y_copy(j).start()
        own_copy(direct(j)).start()
    for j in range(HALF):
        load_tok(swapped(j)).wait()
        own_copy(swapped(j)).start()
    for cp in load_w(direct(0), 0) + load_w(swapped(0), 1):
        cp.start()
    for i in range(4):
        load_wd(i).start()

    lane = lax.broadcasted_iota(jnp.int32, (rows, 128), 1)
    first = ids_ref[:, 0:1] == lane
    second = ids_ref[:, 1:2] == lane
    named = jnp.where(first | second, 1.0, 0.0).astype(F32)
    weight = jnp.where(first, gates_ref[:, 0:1], jnp.where(second, gates_ref[:, 1:2], 0.0))
    tri_r = lax.broadcasted_iota(jnp.int32, (rows, rows), 0)
    tri_c = lax.broadcasted_iota(jnp.int32, (rows, rows), 1)
    before = jnp.where(tri_c < tri_r, 1.0, 0.0).astype(BF16)
    position = jnp.dot(before, named.astype(BF16), preferred_element_type=F32)
    slot = jnp.where(named > 0.5, position + ((lane % experts) * CAP).astype(F32), -1.0)
    slot_t = slot.T
    weight_t = weight.T
    for e in range(4):
        meta[e, 0:experts, :] = slot_t[e * experts:(e + 1) * experts, :]
        meta[e, experts:2 * experts, :] = weight_t[e * experts:(e + 1) * experts, :]
    for k, e in enumerate(peers):
        meta_copy(e, k).start()
    meta_in[ep] = meta[ep]
    acc[...] = jnp.zeros_like(acc)
    for k, e in enumerate(peers):
        meta_arrive(e, k).wait_recv()

    row_f = tri_r.astype(F32)
    for s in range(4):
        info = meta_in[s]
        put = jnp.zeros((rows, rows), F32)
        for e in range(experts):
            put += jnp.where(row_f == info[e:e + 1, :], 1.0, 0.0)
        place[s] = put.astype(BF16)
        collect[s] = put.T.astype(BF16)
        for e in range(experts):
            g = jnp.sum(
                put[e * CAP:(e + 1) * CAP, :] * info[experts + e:experts + e + 1, :],
                axis=1, keepdims=True)
            rowg[e, s * CAP:(s + 1) * CAP, :] = jnp.broadcast_to(g, (CAP, 128))

    def work(ch, slot_no):
        for s in range(4):
            x = jnp.dot(place[s], tok[ch, s], preferred_element_type=F32).astype(BF16)
            for e in range(experts):
                xr[e, s * CAP:(s + 1) * CAP, :] = x[e * CAP:(e + 1) * CAP, :]
        for cp in load_w(ch, slot_no):
            cp.wait()

        def one(e, carry):
            for k in range(2):
                acc[k, e] += jnp.dot(xr[e], wbuf[slot_no, k, e], preferred_element_type=F32)
            return carry
        lax.fori_loop(0, experts, one, 0)

    def step(j, carry):
        @pl.when(j < HALF)
        def _():
            y_arrive(j).wait_recv()
            z_copy(j).start()
            fwd_copy(direct(j)).start()

        @pl.when(j >= 1)
        def _():
            z_arrive(j - 1).wait_recv()
            fwd_copy(swapped(j - 1)).start()

        @pl.when(j < HALF)
        def _():
            ch = direct(j)
            own_arrive(ch).wait_recv()
            fwd_arrive(ch).wait_recv()
            work(ch, 0)

            @pl.when(j < HALF - 1)
            def _():
                for cp in load_w(direct(j + 1), 0):
                    cp.start()

        @pl.when(j >= 1)
        def _():
            ch = swapped(j - 1)
            own_arrive(ch).wait_recv()
            fwd_arrive(ch).wait_recv()
            work(ch, 1)

            @pl.when(j < HALF)
            def _():
                for cp in load_w(swapped(j), 1):
                    cp.start()
        return carry
    lax.fori_loop(0, HALF + 1, step, 0)

    def activate(e, carry):
        g = acc[0, e]
        h = g / (1.0 + jnp.exp(-g)) * acc[1, e]
        hid[e] = (h * rowg[e][:, 0:1]).astype(BF16)
        return carry
    lax.fori_loop(0, experts, activate, 0)

    def core_copy(i):
        return remote(part.at[i, 1 - c], core_in.at[i], pc_send.at[i], pc_recv.at[i], partner, z)

    def ret_copy(i):
        return remote(part.at[i, c, 1 - y], y_in.at[i], py_send.at[i], py_recv.at[i], across, z)

    def scatter_copy(i):
        q = (z + Z_OFFSETS[i]) % 4
        return remote(part.at[i, c, y], z_in.at[i], pz_send.at[i], pz_recv.at[i], ep, q)

    for i in range(5):
        if i < 4:
            load_wd(i).wait()

            def down(e, carry):
                o = jnp.dot(hid[e], wd[i, e], preferred_element_type=F32).astype(BF16)
                for s in range(4):
                    dnb[s, span(e, CAP), :] = o[s * CAP:(s + 1) * CAP, :]
                return carry
            lax.fori_loop(0, experts, down, 0)

            def gather(s, carry):
                part[i, s % 2, s // 2] = jnp.dot(
                    collect[s], dnb[s], preferred_element_type=F32).astype(BF16)
                return carry
            lax.fori_loop(0, 4, gather, 0)
            core_copy(i).start()
        if i >= 1:
            core_copy(i - 1).wait_recv()
            part[i - 1, c, 1 - y] += core_in[i - 1, 1 - y]
            ret_copy(i - 1).start()

    for i in range(3):
        ret_copy(i).wait_recv()
        part[i, c, y] += core_in[i, y] + y_in[i]
        scatter_copy(i).start()
    ret_copy(3).wait_recv()
    total = (part[3, c, y] + core_in[3, y] + y_in[3]).astype(F32)
    for i in range(3):
        scatter_copy(i).wait_recv()
        total += z_in[i].astype(F32)

    local_mean = jnp.sum(total, axis=1, keepdims=True) * (1.0 / piece)
    gap = total - local_mean
    local_m2 = jnp.sum(gap * gap, axis=1, keepdims=True)
    mean_t = jnp.broadcast_to(local_mean, (rows, 128)).T
    m2_t = jnp.broadcast_to(local_m2, (rows, 128)).T
    st_out[0:8, :] = mean_t[0:8, :]
    st_out[8:16, :] = m2_t[0:8, :]

    def stat_copy(d):
        return remote(
            st_out, st_in.at[d - 1], st_send.at[d - 1], st_recv.at[d - 1], ep, (z + d) % 4)
    for d in (1, 2, 3):
        stat_copy(d).start()
    for d in (1, 2, 3):
        stat_copy(d).wait_recv()
    means = [st_out[0:8, :]] + [st_in[d, 0:8, :] for d in range(3)]
    m2s = [st_out[8:16, :]] + [st_in[d, 8:16, :] for d in range(3)]
    mean = (means[0] + means[1] + means[2] + means[3]) * 0.25
    m2 = m2s[0] + m2s[1] + m2s[2] + m2s[3]
    for m in means:
        m2 += (m - mean) * (m - mean) * piece
    scale = lax.rsqrt(m2 * (1.0 / width) + norm_eps)
    mean_col = jnp.broadcast_to(mean[0:1, :], (128, rows)).T[:, 0:1]
    scale_col = jnp.broadcast_to(scale[0:1, :], (128, rows)).T[:, 0:1]
    out_ref[...] = (
        (total - mean_col) * scale_col * gain_ref[...] + bias_ref[...]).astype(BF16)

    for j in range(HALF):
        y_copy(j).wait_send()
        z_copy(j).wait_send()
    for ch in range(CHUNKS):
        own_copy(ch).wait_send()
        fwd_copy(ch).wait_send()
    for k, e in enumerate(peers):
        meta_copy(e, k).wait_send()
    for i in range(4):
        core_copy(i).wait_send()
        ret_copy(i).wait_send()
    for i in range(3):
        scatter_copy(i).wait_send()
    for d in (1, 2, 3):
        stat_copy(d).wait_send()


def fused_on_device(tokens, expert_ids, gates, w_gate, w_up, w_down, norm_gain, norm_bias):
    rows, width = tokens.shape
    experts, _, hidden = w_gate.shape
    piece = norm_gain.shape[0]
    cols = width // CHUNKS
    dma = pltpu.SemaphoreType.DMA
    vmem = pl.BlockSpec(memory_space=pltpu.VMEM)
    hbm = pl.BlockSpec(memory_space=pl.ANY)
    return pl.pallas_call(
        moe_kernel,
        out_shape=jax.ShapeDtypeStruct((rows, piece), jnp.bfloat16),
        in_specs=[vmem] * 4 + [hbm] * 4,
        out_specs=vmem,
        scratch_shapes=[
            pltpu.VMEM((CHUNKS, 4, rows, cols), BF16),
            pltpu.VMEM((2, 2, experts, cols, hidden), BF16),
            pltpu.VMEM((4, experts, hidden, piece), BF16),
            pltpu.VMEM((2, experts, 4 * CAP, hidden), F32),
            pltpu.VMEM((experts, 4 * CAP, hidden), BF16),
            pltpu.VMEM((experts, 4 * CAP, cols), BF16),
            pltpu.VMEM((4, experts * CAP, piece), BF16),
            pltpu.VMEM((4, experts * CAP, rows), BF16),
            pltpu.VMEM((4, rows, experts * CAP), BF16),
            pltpu.VMEM((experts, 4 * CAP, 128), F32),
            pltpu.VMEM((4, 2 * experts, rows), F32),
            pltpu.VMEM((4, 2 * experts, rows), F32),
            pltpu.VMEM((4, 2, 2, rows, piece), BF16),
            pltpu.VMEM((4, 2, rows, piece), BF16),
            pltpu.VMEM((4, rows, piece), BF16),
            pltpu.VMEM((3, rows, piece), BF16),
            pltpu.VMEM((16, rows), F32),
            pltpu.VMEM((3, 16, rows), F32),
            dma((CHUNKS,)), dma((HALF,)), dma((HALF,)), dma((HALF,)), dma((HALF,)),
            dma((CHUNKS,)), dma((CHUNKS,)), dma((CHUNKS,)), dma((CHUNKS,)),
            dma((3,)), dma((3,)), dma((2, 2)), dma((4,)),
            dma((4,)), dma((4,)), dma((4,)), dma((4,)),
            dma((3,)), dma((3,)), dma((3,)), dma((3,)),
        ],
        compiler_params=pltpu.CompilerParams(
            collective_id=0, has_side_effects=True, vmem_limit_bytes=64 * 1024 * 1024 - 65536),
    )(
        expert_ids, gates, norm_gain[None, :], norm_bias[None, :],
        tokens, w_gate, w_up, w_down,
    )


def solution(mesh):
    groups_apart = EXPERTS == GROUP_EXPERTS * mesh.shape["ep"]
    fused = groups_apart and mesh.shape["ep"] == 4 and mesh.shape["tp"] == 4
    return jax.shard_map(
        fused_on_device if fused else on_device,
        mesh=mesh,
        in_specs=(
            P(("grp", "ep"), None),
            P(("grp", "ep"), None),
            P(("grp", "ep"), None),
            P("ep", None, "tp"),
            P("ep", None, "tp"),
            P("ep", "tp", None),
            P("tp"),
            P("tp"),
        ),
        out_specs=P(("grp", "ep"), "tp"),
        check_vma=False,
    )
```

```python
import functools
import jax
import jax.numpy as jnp
from jax import lax
from jax.experimental import pallas as pl
from jax.experimental.pallas import tpu as pltpu
from jax.sharding import PartitionSpec as P

D = 4096
TOPK = 2
EXPERTS = 16
CAP = 64


norm_eps = 1e-05


def route_slots(expert_ids):
    flat_ids = expert_ids.reshape(-1)
    onehot = (flat_ids[:, None] == jnp.arange(EXPERTS, dtype=jnp.int32)[None, :]).astype(jnp.int32)
    position = jnp.sum((jnp.cumsum(onehot, axis=0) - 1) * onehot, axis=1)
    target = flat_ids * CAP + position
    token_of = jnp.arange(flat_ids.shape[0], dtype=jnp.int32) // TOPK
    source = jnp.zeros((EXPERTS * CAP,), jnp.int32).at[target].set(token_of)
    filled = jnp.zeros((EXPERTS * CAP,), jnp.bool_).at[target].set(True)
    return (target, source, filled)


def on_device(tokens, expert_ids, gates, w_gate, w_up, w_down, norm_gain, norm_bias):
    tok_rows, width = tokens.shape
    piece_width = norm_gain.shape[0]
    target, source, filled = route_slots(expert_ids)
    outgoing = jnp.where(filled[:, None], tokens[source], jnp.zeros((), jnp.bfloat16)).reshape(
        EXPERTS, CAP, width
    )
    arrived = lax.all_to_all(outgoing, "ep", split_axis=0, concat_axis=1, tiled=True)
    gate_part = jnp.einsum("erd,edf->erf", arrived, w_gate, preferred_element_type=jnp.float32)
    up_part = jnp.einsum("erd,edf->erf", arrived, w_up, preferred_element_type=jnp.float32)
    hidden = (jax.nn.silu(gate_part) * up_part).astype(jnp.bfloat16)
    partial_value = jnp.einsum("erf,efd->erd", hidden, w_down, preferred_element_type=jnp.float32)
    summed = lax.psum_scatter(
        partial_value.astype(jnp.bfloat16), "tp", scatter_dimension=2, tiled=True
    )
    returned = lax.all_to_all(summed, "ep", split_axis=1, concat_axis=0, tiled=True)
    picked = returned.reshape(EXPERTS * CAP, piece_width)[target].reshape(
        tok_rows, TOPK, piece_width
    )
    combined = jnp.sum(picked.astype(jnp.float32) * gates[:, :, None], axis=1)
    stats = lax.psum((jnp.sum(combined, axis=1), jnp.sum(combined * combined, axis=1)), "tp")
    row_mean = stats[0] / D
    row_var = stats[1] / D - row_mean * row_mean
    normed = (combined - row_mean[:, None]) * lax.rsqrt(
        row_var[:, None] + norm_eps
    ) * norm_gain + norm_bias
    return normed.astype(jnp.bfloat16)


GROUP_EXPERTS = 4
CHUNKS = 16
HALF = CHUNKS // 2
Z_OFFSETS = (2, 2, 1, 1, 3, 3, 0, 0)
PIECES = 8
SENT = 6
LAG = 4
F32 = jnp.float32
BF16 = jnp.bfloat16
MESH = pl.DeviceIdType.MESH


def moe_kernel(
    ids_ref, gates_ref, gain_ref, bias_ref, tokens_ref, wg_ref, wu_ref, wd_ref,
    out_ref,
    tok, wbuf, wd, acc, hid, xr, dnb, place, collect, rowg, meta, meta_in,
    part, core_in, y_in, z_in, st_out, st_in,
    tok_sem, y_send, y_recv, z_send, z_recv, own_send, own_recv, fwd_send, fwd_recv,
    meta_send, meta_recv, w_sem, wd_sem, pc_send, pc_recv, py_send, py_recv,
    pz_send, pz_recv, st_send, st_recv,
):
    ep = lax.axis_index("ep")
    z = lax.axis_index("tp")
    y, c = ep // 2, ep % 2
    partner = y * 2 + (1 - c)
    across = (1 - y) * 2 + c
    diag = (1 - y) * 2 + (1 - c)
    par = z % 2
    zpeer = z + 1 - 2 * par
    rows, width = tokens_ref.shape
    experts = wg_ref.shape[0]
    cols = width // CHUNKS
    piece = gain_ref.shape[1]
    part_cols = piece // 2

    def remote(src, dst, send, recv, e, t):
        return pltpu.make_async_remote_copy(
            src_ref=src, dst_ref=dst, send_sem=send, recv_sem=recv,
            device_id={"ep": e, "tp": t}, device_id_type=MESH,
        )

    def span(ch, size):
        return pl.ds(pl.multiple_of(ch * size, size), size)

    def load_tok(ch):
        return pltpu.make_async_copy(
            tokens_ref.at[:, span(ch, cols)], tok.at[ch, ep], tok_sem.at[ch])

    def load_w(ch, slot):
        return (
            pltpu.make_async_copy(
                wg_ref.at[:, span(ch, cols), :], wbuf.at[slot, 0], w_sem.at[slot, 0]),
            pltpu.make_async_copy(
                wu_ref.at[:, span(ch, cols), :], wbuf.at[slot, 1], w_sem.at[slot, 1]),
        )

    def load_wd(i):
        q = (z + Z_OFFSETS[i]) % 4
        return pltpu.make_async_copy(
            wd_ref.at[:, :, span(q * 2 + i % 2, part_cols)], wd.at[i], wd_sem.at[i])

    def direct(j):
        return par * HALF + j

    def swapped(j):
        return (1 - par) * HALF + j

    def y_copy(j):
        blk = tok.at[direct(j), ep]
        return remote(blk, blk, y_send.at[j], y_recv.at[j], across, z)

    def y_arrive(j):
        blk = tok.at[direct(j), across]
        return remote(blk, blk, y_send.at[j], y_recv.at[j], across, z)

    def z_copy(j):
        blk = tok.at[direct(j), across]
        return remote(blk, blk, z_send.at[j], z_recv.at[j], ep, zpeer)

    def z_arrive(j):
        blk = tok.at[swapped(j), across]
        return remote(blk, blk, z_send.at[j], z_recv.at[j], ep, zpeer)

    def own_copy(ch):
        blk = tok.at[ch, ep]
        return remote(blk, blk, own_send.at[ch], own_recv.at[ch], partner, z)

    def own_arrive(ch):
        blk = tok.at[ch, partner]
        return remote(blk, blk, own_send.at[ch], own_recv.at[ch], partner, z)

    def fwd_copy(ch):
        blk = tok.at[ch, across]
        return remote(blk, blk, fwd_send.at[ch], fwd_recv.at[ch], partner, z)

    def fwd_arrive(ch):
        blk = tok.at[ch, diag]
        return remote(blk, blk, fwd_send.at[ch], fwd_recv.at[ch], partner, z)

    def meta_copy(e, k):
        return remote(meta.at[e], meta_in.at[ep], meta_send.at[k], meta_recv.at[k], e, z)

    def meta_arrive(e, k):
        return remote(meta.at[e], meta_in.at[e], meta_send.at[k], meta_recv.at[k], e, z)

    peers = (partner, across, diag)

    for j in range(HALF):
        load_tok(direct(j)).start()
    for j in range(HALF):
        load_tok(swapped(j)).start()

    barrier = pltpu.get_barrier_semaphore()
    for e in peers:
        pl.semaphore_signal(barrier, inc=1, device_id={"ep": e, "tp": z}, device_id_type=MESH)
    for d in (1, 2, 3):
        pl.semaphore_signal(
            barrier, inc=1, device_id={"ep": ep, "tp": (z + d) % 4}, device_id_type=MESH)
    total_experts = 4 * experts
    expert_row = lax.broadcasted_iota(jnp.int32, (total_experts, rows), 0)
    first = ids_ref[0:1, :] == expert_row
    second = ids_ref[1:2, :] == expert_row
    named = jnp.where(first | second, 1.0, 0.0).astype(F32)
    weight = jnp.where(first, gates_ref[0:1, :], jnp.where(second, gates_ref[1:2, :], 0.0))
    tri_r = lax.broadcasted_iota(jnp.int32, (rows, rows), 0)
    tri_c = lax.broadcasted_iota(jnp.int32, (rows, rows), 1)
    before = jnp.where(tri_r < tri_c, 1.0, 0.0).astype(BF16)
    position = jnp.dot(named.astype(BF16), before, preferred_element_type=F32)
    slot = jnp.where(
        named > 0.5, position + ((expert_row % experts) * CAP).astype(F32), -1.0)
    for e in range(4):
        meta[e, 0:experts, :] = slot[e * experts:(e + 1) * experts, :]
        meta[e, experts:2 * experts, :] = weight[e * experts:(e + 1) * experts, :]
    pl.semaphore_wait(barrier, 6)
    for k, e in enumerate(peers):
        meta_copy(e, k).start()

    for j in range(HALF):
        load_tok(direct(j)).wait()
        y_copy(j).start()
        own_copy(direct(j)).start()
    for j in range(HALF):
        load_tok(swapped(j)).wait()
        own_copy(swapped(j)).start()
    for cp in load_w(direct(0), 0) + load_w(swapped(0), 1):
        cp.start()
    for i in range(PIECES):
        load_wd(i).start()

    meta_in[ep] = meta[ep]
    acc[...] = jnp.zeros_like(acc)
    for k, e in enumerate(peers):
        meta_arrive(e, k).wait_recv()

    row_f = tri_r.astype(F32)
    for s in range(4):
        info = meta_in[s]
        put = jnp.zeros((rows, rows), F32)
        for e in range(experts):
            put += jnp.where(row_f == info[e:e + 1, :], 1.0, 0.0)
        place[s] = put.astype(BF16)
        collect[s] = put.T.astype(BF16)
        for e in range(experts):
            g = jnp.sum(
                put[e * CAP:(e + 1) * CAP, :] * info[experts + e:experts + e + 1, :],
                axis=1, keepdims=True)
            rowg[e, s * CAP:(s + 1) * CAP, :] = jnp.broadcast_to(g, (CAP, 128))

    def work(ch, slot_no):
        for s in range(4):
            x = jnp.dot(place[s], tok[ch, s], preferred_element_type=F32).astype(BF16)
            for e in range(experts):
                xr[e, s * CAP:(s + 1) * CAP, :] = x[e * CAP:(e + 1) * CAP, :]
        for cp in load_w(ch, slot_no):
            cp.wait()

        def one(e, carry):
            for k in range(2):
                acc[k, e] += jnp.dot(xr[e], wbuf[slot_no, k, e], preferred_element_type=F32)
            return carry
        lax.fori_loop(0, experts, one, 0)

    def step(j, carry):
        @pl.when(j < HALF)
        def _():
            y_arrive(j).wait_recv()
            z_copy(j).start()
            fwd_copy(direct(j)).start()

        @pl.when(j >= 1)
        def _():
            z_arrive(j - 1).wait_recv()
            fwd_copy(swapped(j - 1)).start()

        @pl.when(j < HALF)
        def _():
            ch = direct(j)
            own_arrive(ch).wait_recv()
            fwd_arrive(ch).wait_recv()
            work(ch, 0)

            @pl.when(j < HALF - 1)
            def _():
                for cp in load_w(direct(j + 1), 0):
                    cp.start()

        @pl.when(j >= 1)
        def _():
            ch = swapped(j - 1)
            own_arrive(ch).wait_recv()
            fwd_arrive(ch).wait_recv()
            work(ch, 1)

            @pl.when(j < HALF)
            def _():
                for cp in load_w(swapped(j), 1):
                    cp.start()
        return carry
    lax.fori_loop(0, HALF + 1, step, 0)

    def activate(e, carry):
        g = acc[0, e]
        h = g / (1.0 + jnp.exp(-g)) * acc[1, e]
        hid[e] = (h * rowg[e][:, 0:1]).astype(BF16)
        return carry
    lax.fori_loop(0, experts, activate, 0)

    def core_copy(i):
        return remote(part.at[i, 1 - c], core_in.at[i], pc_send.at[i], pc_recv.at[i], partner, z)

    def ret_copy(i):
        return remote(part.at[i, c, 1 - y], y_in.at[i], py_send.at[i], py_recv.at[i], across, z)

    def scatter_copy(i):
        q = (z + Z_OFFSETS[i]) % 4
        return remote(part.at[i, c, y], z_in.at[i], pz_send.at[i], pz_recv.at[i], ep, q)

    for i in range(PIECES + LAG):
        if i < PIECES:
            load_wd(i).wait()

            def down(e, carry):
                o = jnp.dot(hid[e], wd[i, e], preferred_element_type=F32).astype(BF16)
                for s in range(4):
                    dnb[s, span(e, CAP), :] = o[s * CAP:(s + 1) * CAP, :]
                return carry
            lax.fori_loop(0, experts, down, 0)

            def gather(s, carry):
                part[i, s % 2, s // 2] = jnp.dot(
                    collect[s], dnb[s], preferred_element_type=F32).astype(BF16)
                return carry
            lax.fori_loop(0, 4, gather, 0)
            core_copy(i).start()
        if 1 <= i <= PIECES:
            core_copy(i - 1).wait_recv()
            part[i - 1, c, 1 - y] += core_in[i - 1, 1 - y]
            ret_copy(i - 1).start()
        if i >= LAG:
            k = i - LAG
            ret_copy(k).wait_recv()
            part[k, c, y] += core_in[k, y] + y_in[k]
            if k < SENT:
                scatter_copy(k).start()

    halves = []
    for h in range(2):
        half = part[SENT + h, c, y].astype(F32)
        for i in range(h, SENT, 2):
            scatter_copy(i).wait_recv()
            half += z_in[i].astype(F32)
        halves.append(half)
    total = jnp.concatenate(halves, axis=1)

    local_mean = jnp.sum(total, axis=1, keepdims=True) * (1.0 / piece)
    gap = total - local_mean
    local_m2 = jnp.sum(gap * gap, axis=1, keepdims=True)
    mean_t = jnp.broadcast_to(local_mean, (rows, 128)).T
    m2_t = jnp.broadcast_to(local_m2, (rows, 128)).T
    st_out[0:8, :] = mean_t[0:8, :]
    st_out[8:16, :] = m2_t[0:8, :]

    def stat_copy(d):
        return remote(
            st_out, st_in.at[d - 1], st_send.at[d - 1], st_recv.at[d - 1], ep, (z + d) % 4)
    for d in (1, 2, 3):
        stat_copy(d).start()
    for d in (1, 2, 3):
        stat_copy(d).wait_recv()
    means = [st_out[0:8, :]] + [st_in[d, 0:8, :] for d in range(3)]
    m2s = [st_out[8:16, :]] + [st_in[d, 8:16, :] for d in range(3)]
    mean = (means[0] + means[1] + means[2] + means[3]) * 0.25
    m2 = m2s[0] + m2s[1] + m2s[2] + m2s[3]
    for m in means:
        m2 += (m - mean) * (m - mean) * piece
    scale = lax.rsqrt(m2 * (1.0 / width) + norm_eps)
    mean_col = jnp.broadcast_to(mean[0:1, :], (128, rows)).T[:, 0:1]
    scale_col = jnp.broadcast_to(scale[0:1, :], (128, rows)).T[:, 0:1]
    out_ref[...] = (
        (total - mean_col) * scale_col * gain_ref[...] + bias_ref[...]).astype(BF16)

    for j in range(HALF):
        y_copy(j).wait_send()
        z_copy(j).wait_send()
    for ch in range(CHUNKS):
        own_copy(ch).wait_send()
        fwd_copy(ch).wait_send()
    for k, e in enumerate(peers):
        meta_copy(e, k).wait_send()
    for i in range(PIECES):
        core_copy(i).wait_send()
        ret_copy(i).wait_send()
    for i in range(SENT):
        scatter_copy(i).wait_send()
    for d in (1, 2, 3):
        stat_copy(d).wait_send()


def fused_on_device(tokens, expert_ids, gates, w_gate, w_up, w_down, norm_gain, norm_bias):
    rows, width = tokens.shape
    experts, _, hidden = w_gate.shape
    piece = norm_gain.shape[0]
    cols = width // CHUNKS
    part_cols = piece // 2
    dma = pltpu.SemaphoreType.DMA
    vmem = pl.BlockSpec(memory_space=pltpu.VMEM)
    hbm = pl.BlockSpec(memory_space=pl.ANY)
    return pl.pallas_call(
        moe_kernel,
        out_shape=jax.ShapeDtypeStruct((rows, piece), jnp.bfloat16),
        in_specs=[vmem] * 4 + [hbm] * 4,
        out_specs=vmem,
        scratch_shapes=[
            pltpu.VMEM((CHUNKS, 4, rows, cols), BF16),
            pltpu.VMEM((2, 2, experts, cols, hidden), BF16),
            pltpu.VMEM((PIECES, experts, hidden, part_cols), BF16),
            pltpu.VMEM((2, experts, 4 * CAP, hidden), F32),
            pltpu.VMEM((experts, 4 * CAP, hidden), BF16),
            pltpu.VMEM((experts, 4 * CAP, cols), BF16),
            pltpu.VMEM((4, experts * CAP, part_cols), BF16),
            pltpu.VMEM((4, experts * CAP, rows), BF16),
            pltpu.VMEM((4, rows, experts * CAP), BF16),
            pltpu.VMEM((experts, 4 * CAP, 128), F32),
            pltpu.VMEM((4, 2 * experts, rows), F32),
            pltpu.VMEM((4, 2 * experts, rows), F32),
            pltpu.VMEM((PIECES, 2, 2, rows, part_cols), BF16),
            pltpu.VMEM((PIECES, 2, rows, part_cols), BF16),
            pltpu.VMEM((PIECES, rows, part_cols), BF16),
            pltpu.VMEM((SENT, rows, part_cols), BF16),
            pltpu.VMEM((16, rows), F32),
            pltpu.VMEM((3, 16, rows), F32),
            dma((CHUNKS,)), dma((HALF,)), dma((HALF,)), dma((HALF,)), dma((HALF,)),
            dma((CHUNKS,)), dma((CHUNKS,)), dma((CHUNKS,)), dma((CHUNKS,)),
            dma((3,)), dma((3,)), dma((2, 2)), dma((PIECES,)),
            dma((PIECES,)), dma((PIECES,)), dma((PIECES,)), dma((PIECES,)),
            dma((SENT,)), dma((SENT,)), dma((3,)), dma((3,)),
        ],
        compiler_params=pltpu.CompilerParams(
            collective_id=0, has_side_effects=True, vmem_limit_bytes=64 * 1024 * 1024 - 65536),
    )(
        expert_ids.T, gates.T, norm_gain[None, :], norm_bias[None, :],
        tokens, w_gate, w_up, w_down,
    )


def solution(mesh):
    groups_apart = EXPERTS == GROUP_EXPERTS * mesh.shape["ep"]
    fused = groups_apart and mesh.shape["ep"] == 4 and mesh.shape["tp"] == 4
    return jax.shard_map(
        fused_on_device if fused else on_device,
        mesh=mesh,
        in_specs=(
            P(("grp", "ep"), None),
            P(("grp", "ep"), None),
            P(("grp", "ep"), None),
            P("ep", None, "tp"),
            P("ep", None, "tp"),
            P("ep", "tp", None),
            P("tp"),
            P("tp"),
        ),
        out_specs=P(("grp", "ep"), "tp"),
        check_vma=False,
    )
```
